32 devices in a mesh: sp: 16 (over z, y, x), tp: 2 (over core).
Axes of the slice: x: 2, y: 2, z: 4, core: 2. Of those that a mesh axis runs over, the one named last changes fastest.
Arguments:
- tokens: bfloat16 [2048, 2048], P('sp', 'tp'), may hold values from -6 to 6
- in_gain: bfloat16 [1, 2048], P(None, 'tp'), may hold values from 0.099609375 to 1.8984375
- w_input: bfloat16 [2048, 1024], P(None, 'tp'), may hold values from -0.125 to 0.125
- w_bgate: bfloat16 [2048, 1024], P(None, 'tp'), may hold values from -0.125 to 0.125
- w_cgate: bfloat16 [2048, 1024], P(None, 'tp'), may hold values from -0.125 to 0.125
- w_value: bfloat16 [2048, 1024], P(None, 'tp'), may hold values from -0.125 to 0.125
- decay_rate: float32 [64, 64], P('tp'), may hold values from 9.765625e-05 to 0.034, as said below
- angle: float32 [64, 64], P('tp'), may hold values from -3.140625 to 3.140625
- decay_shift: float32 [64, 2048], P('tp', 'sp'), may hold values from -1.1 to 0, as said below
- b_input: float32 [2, 64, 64, 16], P(None, 'tp'), may hold values from -1 to 1
- c_output: float32 [2, 64, 16, 64], P(None, 'tp'), may hold values from -0.75 to 0.75
- initial_recurrence_vector: float32 [2, 64, 64], P(None, 'tp'), may hold values from -271.529 to 271.529
- skip_gain: float32 [1024], P('tp'), may hold values from -4 to 4
- ssm_gain: float32 [1024], P('tp'), may hold values from 0.1 to 1.9
- conv_gain: float32 [1024], P('tp'), may hold values from 0.1 to 1.9
- conv_taps: float32 [3, 1024], P(None, 'tp'), may hold values from -3.5 to 3.5
- w_out_ssm: bfloat16 [1024, 2048], P('tp'), may hold values from -0.125 to 0.125
- w_out_conv: bfloat16 [1024, 2048], P('tp'), may hold values from -0.125 to 0.125
Outputs:
- mixed: bfloat16 [2048, 2048], P(('sp', 'tp'))
The draws below stay inside these ranges and needn't reach their ends.
Inputs may be any that keep to these rules, and one draw needn't show every extreme that they name: `decay_rate`: positive rates. `decay_shift`: never positive.
All inputs are finite; a program needn't handle non-finite values.
Results may differ from the reference program's by a relative error of at most 0.0085.
Values may be sent and summed in bfloat16 or wider, within the bound.
A program may use at most 64 MiB of HBM per device.

```python
import math
import jax
import jax.numpy as jnp
from jax import lax

D = 2048
SSM_GROUPS = 64
GROUP_CH = 16
STATE = 64
CONVOLUTION_CHAN = 64
KERNEL = 3
TOK_DEV = 128
TOKENS = 2048
D_SSM = 1024
D_CONV = 1024
N_TP = 2


def slow_groups(key):
    share = 0.5
    return jax.random.uniform(jax.random.fold_in(key, 11), (SSM_GROUPS,), jnp.float32) < share


def draw_decay_rate(key, part):
    slow = slow_groups(key)
    spread = jax.random.uniform(jax.random.fold_in(key, 12), (SSM_GROUPS, STATE), jnp.float32)
    slow_rate = (0.2 + 0.3 * spread) / TOKENS
    fast_rate = jnp.exp(math.log(0.01) + spread * (math.log(1.0 / 30.0) - math.log(0.01)))
    return jnp.where(slow[:, None], slow_rate, fast_rate).astype(jnp.float32)


def draw_decay_shift(key, part):
    slow = slow_groups(key)
    factor = jax.random.uniform(jax.random.fold_in(key, 13), (SSM_GROUPS, TOKENS // TOK_DEV), jnp.float32)
    level = jnp.where(slow, 0.5 / TOKENS, 1.0 / 60.0)
    starting_shift_amount = -jnp.repeat(factor * level[:, None], TOK_DEV, axis=1)
    slot_numbers_list = jax.random.randint(jax.random.fold_in(key, 14), (SSM_GROUPS, 2), 0, TOKENS)
    objective_errors = jax.random.uniform(jax.random.fold_in(key, 15), (SSM_GROUPS, 2), jnp.float32, 0.2, 0.4)
    sequence_slot_number = jnp.arange(TOKENS)[None, :]
    symbol_batches_count = jnp.where(sequence_slot_number == slot_numbers_list[:, 0:1], jnp.log(1.0 - objective_errors[:, 0:1]), 0.0)
    symbol_batches_count = symbol_batches_count + jnp.where(sequence_slot_number == slot_numbers_list[:, 1:2], jnp.log(1.0 - objective_errors[:, 1:2]), 0.0)
    return (starting_shift_amount + symbol_batches_count).astype(jnp.float32)


def steps_of(own_key, dims, cuts, smallest, largest):
    level, own = 1.0, jax.random.fold_in(own_key, 6)
    for position, shards_of in cuts:
        draws = jnp.exp(jax.random.uniform(jax.random.fold_in(own, position), (shards_of,), jnp.float32, smallest / len(cuts), largest / len(cuts)))
        level = level * jnp.repeat(draws, dims[position] // shards_of).reshape([-1 if axis == position else 1 for axis in range(len(dims))])
    return level


def noise(rng, dims, scale, limit, cuts=(), held_as=jnp.bfloat16):
    loudness = steps_of(rng, dims, cuts, -0.22, 0.18) if cuts else 1.0
    drawn = jax.random.normal(rng, dims, jnp.float32) * scale * loudness
    return jnp.minimum(jnp.maximum(drawn, -limit), limit).astype(held_as)


def setup_inputs(seed: int = 0) -> dict:
    streams_of = jax.random.split(jax.random.key(seed), 19)
    return {
        "tokens": noise(streams_of[0], (TOKENS, D), 1.0, 6.0, ((0, 16), (1, 2))),
        "in_gain": jnp.clip(1.0 + 0.18 * jax.random.normal(streams_of[1], (1, D), jnp.float32), 0.099609375, 1.8984375).astype(jnp.bfloat16),
        "w_input": noise(streams_of[2], (D, D_SSM), D ** -0.5, 0.125, ((1, 2),)),
        "w_bgate": noise(streams_of[3], (D, D_CONV), D ** -0.5, 0.125, ((1, 2),)),
        "w_cgate": noise(streams_of[4], (D, D_CONV), D ** -0.5, 0.125, ((1, 2),)),
        "w_value": noise(streams_of[5], (D, D_CONV), D ** -0.5, 0.125, ((1, 2),)),
        "decay_rate": draw_decay_rate(jax.random.fold_in(streams_of[18], 71), 0),
        "angle": jnp.clip(jax.random.uniform(streams_of[7], (SSM_GROUPS, STATE), jnp.float32, -3.140625, 3.140625), -3.140625, 3.140625),
        "decay_shift": draw_decay_shift(jax.random.fold_in(streams_of[18], 71), 0),
        "b_input": noise(streams_of[9], (2, SSM_GROUPS, STATE, GROUP_CH), (2 * GROUP_CH) ** -0.5, 1.0, ((1, 2),), jnp.float32),
        "c_output": noise(streams_of[10], (2, SSM_GROUPS, GROUP_CH, STATE), STATE ** -0.5, 0.75, ((1, 2),), jnp.float32),
        "initial_recurrence_vector": noise(streams_of[11], (2, SSM_GROUPS, STATE), (TOKENS ** 0.5), 271.529, ((1, 2),), jnp.float32),
        "skip_gain": noise(streams_of[12], (D_SSM,), 1.0, 4.0, ((0, 2),), jnp.float32),
        "ssm_gain": jnp.clip(1.0 + 0.18 * jax.random.normal(streams_of[13], (D_SSM,), jnp.float32), 0.1, 1.9),
        "conv_gain": jnp.clip(1.0 + 0.18 * jax.random.normal(streams_of[14], (D_CONV,), jnp.float32), 0.1, 1.9),
        "conv_taps": noise(streams_of[15], (KERNEL, D_CONV), KERNEL ** -0.5, 3.5, ((1, 2),), jnp.float32),
        "w_out_ssm": noise(streams_of[16], (D_SSM, D), (D_SSM + D_CONV) ** -0.5, 0.125, ((0, 2),)),
        "w_out_conv": noise(streams_of[17], (D_CONV, D), (D_SSM + D_CONV) ** -0.5, 0.125, ((0, 2),)),
    }


def complex_step(first, second):
    ar1, ai1, br1, bi1 = first
    ar2, ai2, br2, bi2 = second
    return (ar2 * ar1 - ai2 * ai1, ar2 * ai1 + ai2 * ar1, ar2 * br1 - ai2 * bi1 + br2, ar2 * bi1 + ai2 * br1 + bi2)

def input_matrix(decay_rate, angle, b_input):
    real_part = jnp.expm1(-decay_rate) * jnp.cos(angle) - 2.0 * jnp.sin(0.5 * angle) ** 2
    imag_part = jnp.exp(-decay_rate) * jnp.sin(angle)
    denom = decay_rate * decay_rate + angle * angle
    zoh_re = (imag_part * angle - real_part * decay_rate) / denom
    zoh_im = -(imag_part * decay_rate + real_part * angle) / denom
    b_re = zoh_re[..., None] * b_input[0] - zoh_im[..., None] * b_input[1]
    b_im = zoh_re[..., None] * b_input[1] + zoh_im[..., None] * b_input[0]
    return (b_re, b_im)

def head_norm(values, gain, width):
    count, total = values.shape
    grouped = values.reshape(count, total // width, width)
    grouped = grouped * lax.rsqrt(lax.optimization_barrier(jnp.mean(grouped * grouped, axis=-1, keepdims=True)) + 1e-06)
    return (grouped.reshape(count, total) * gain).astype(jnp.bfloat16)

def reference(tokens, in_gain, w_input, w_bgate, w_cgate, w_value, decay_rate, angle, decay_shift, b_input, c_output, initial_recurrence_vector, skip_gain, ssm_gain, conv_gain, conv_taps, w_out_ssm, w_out_conv):
    highest = lax.Precision.HIGHEST
    floats = tokens.astype(jnp.float32)
    inv = lax.rsqrt(lax.optimization_barrier(jnp.mean(floats * floats, axis=-1, keepdims=True)) + 1e-06)
    scaled = (floats * in_gain[0].astype(jnp.float32)).astype(jnp.bfloat16)
    u_in = (jnp.dot(scaled, w_input, preferred_element_type=jnp.float32) * inv).astype(jnp.bfloat16)
    bgate = (jnp.dot(scaled, w_bgate, preferred_element_type=jnp.float32) * inv).astype(jnp.bfloat16)
    cgate = (jnp.dot(scaled, w_cgate, preferred_element_type=jnp.float32) * inv).astype(jnp.bfloat16)
    value = (jnp.dot(scaled, w_value, preferred_element_type=jnp.float32) * inv).astype(jnp.bfloat16)
    b_re, b_im = input_matrix(decay_rate, angle, b_input)
    u_groups = u_in.astype(jnp.float32).reshape(TOKENS, SSM_GROUPS, GROUP_CH).transpose(1, 0, 2)

    def single_group(items):
        u_grp, rate, theta, shift, bre, bim, c_re, c_im, init_re, init_im = items
        drive_re = jnp.dot(u_grp, bre.T, precision=highest)
        drive_im = jnp.dot(u_grp, bim.T, precision=highest)
        magnitude = jnp.exp(shift[:, None] - rate[None, :])
        step_re = magnitude * jnp.cos(theta)[None, :]
        step_im = magnitude * jnp.sin(theta)[None, :]
        cum = lax.associative_scan(complex_step, (step_re, step_im, drive_re, drive_im), axis=0)
        state_re = cum[2] + cum[0] * init_re[None, :] - cum[1] * init_im[None, :]
        state_im = cum[3] + cum[0] * init_im[None, :] + cum[1] * init_re[None, :]
        return jnp.dot(state_re, c_re.T, precision=highest) - jnp.dot(state_im, c_im.T, precision=highest)
    outputs = lax.map(single_group, (u_groups, decay_rate, angle, decay_shift, b_re, b_im, c_output[0], c_output[1], initial_recurrence_vector[0], initial_recurrence_vector[1]))
    ssm_pre = outputs.transpose(1, 0, 2).reshape(TOKENS, D_SSM) + skip_gain * u_in.astype(jnp.float32)
    state_space_output = head_norm(jax.nn.gelu(ssm_pre, approximate=False), ssm_gain, GROUP_CH)
    gated = cgate.astype(jnp.float32) * value.astype(jnp.float32)
    padded = jnp.concatenate([jnp.zeros((KERNEL - 1, D_CONV), jnp.float32), gated], axis=0)
    conv = padded[0:TOKENS] * conv_taps[0]
    for tap in range(1, KERNEL):
        conv = conv + padded[tap:tap + TOKENS] * conv_taps[tap]
    conv_out = head_norm(bgate.astype(jnp.float32) * conv, conv_gain, CONVOLUTION_CHAN)
    ssm_width = D_SSM // N_TP
    filter_tap_length = D_CONV // N_TP
    total = jnp.zeros((TOKENS, D), jnp.float32)
    for block in range(N_TP):
        lo = block * ssm_width
        start = block * filter_tap_length
        partial_sum = jnp.dot(state_space_output[:, lo:lo + ssm_width], w_out_ssm[lo:lo + ssm_width], preferred_element_type=jnp.float32)
        partial_sum = partial_sum + jnp.dot(conv_out[:, start:start + filter_tap_length], w_out_conv[start:start + filter_tap_length], preferred_element_type=jnp.float32)
        rounded = lax.optimization_barrier(partial_sum.astype(jnp.bfloat16))
        total = total + rounded.astype(jnp.float32)
    return total.astype(jnp.bfloat16)
```

```python
import functools

import jax
import jax.numpy as jnp
from jax import lax
from jax.experimental import pallas as pl
from jax.experimental.pallas import tpu as pltpu
from jax.sharding import PartitionSpec as P

CONVOLUTION_CHAN = 64
KERNEL = 3
MESH = pl.DeviceIdType.MESH
F32 = jnp.float32
BF16 = jnp.bfloat16


def inner_size(count):
    size = 1
    while size * size < count:
        size *= 2
    return size


def dot(a, b):
    return jnp.dot(a, b, preferred_element_type=F32)


def dot_nt(a, b):
    return lax.dot_general(a, b, (((1,), (1,)), ((), ())), preferred_element_type=F32)


def expm1_of(x):
    series = x * (1 + x / 2 * (1 + x / 3 * (1 + x / 4 * (1 + x / 5 * (1 + x / 6)))))
    return jnp.where(jnp.abs(x) < 0.125, series, jnp.exp(x) - 1)


def zoh_of(rate, angle):
    real_part = expm1_of(-rate) * jnp.cos(angle) - 2.0 * jnp.sin(0.5 * angle) ** 2
    imag_part = jnp.exp(-rate) * jnp.sin(angle)
    denom = rate * rate + angle * angle
    return (
        (imag_part * angle - real_part * rate) / denom,
        -(imag_part * rate + real_part * angle) / denom,
    )


def split3(x):
    hi = x.astype(BF16).astype(F32)
    mid = (x - hi).astype(BF16).astype(F32)
    return hi, mid, x - hi - mid


def kernel(
    sizes,
    tok_h, gain, w_in_h, w_bg_h, w_cg_h, w_va_h, rate, angle, shift, b_in, c_out, init,
    skip, sgain, cgain, taps, wos_h, woc_h,
    out,
    tok, gain_o, w, wos, woc, sc, bx, cx, e_s, d_re, d_im, gated, halo, acc, ssm_b,
    mine1, slots1, mine2, slots2, part_s, part_r,
    loc_sem, tok_send, tok_recv, ph1_send, ph1_recv, ph2_send, ph2_recv, halo_send, halo_recv,
    out_send, out_recv,
):
    nsp, n1, n2 = sizes
    sp, tp = lax.axis_index("sp"), lax.axis_index("tp")
    rows, half = tok_h.shape
    groups, entries = rate.shape
    ch = c_out.shape[2]
    per = 128 // ch
    width = groups * entries
    lines = width // 128
    blocks = groups // per
    wide = per * entries
    inner, outer = lax.rem(sp, n1), lax.div(sp, n1)
    nxt, prv = lax.rem(sp + 1, nsp), lax.rem(sp + nsp - 1, nsp)

    def half_of(ref, which):
        start = (tp if which == 0 else 1 - tp) * half
        return ref.at[pl.ds(pl.multiple_of(start, half), half), :]

    copies = [pltpu.make_async_copy(tok_h, tok.at[0], loc_sem.at[0])]
    for number, ref in enumerate((w_in_h, w_cg_h, w_va_h, w_bg_h)):
        for which in range(2):
            copies.append(
                pltpu.make_async_copy(
                    half_of(ref, which), w.at[number, which], loc_sem.at[len(copies)]
                )
            )
    copies.append(pltpu.make_async_copy(woc_h, woc, loc_sem.at[len(copies)]))
    copies.append(pltpu.make_async_copy(wos_h, wos, loc_sem.at[len(copies)]))
    for copy in copies:
        copy.start()

    peers1 = [outer * n1 + lax.rem(inner + k, n1) for k in range(1, n1)]
    peers2 = [lax.rem(outer + k, n2) * n1 + inner for k in range(1, n2)]
    barrier = pltpu.get_barrier_semaphore()
    pl.semaphore_signal(barrier, inc=1, device_id={"tp": 1 - tp}, device_id_type=MESH)
    for peer in peers1 + peers2 + [nxt, prv]:
        pl.semaphore_signal(barrier, inc=1, device_id={"sp": peer}, device_id_type=MESH)
    pl.semaphore_wait(barrier, 1 + len(peers1) + len(peers2) + 2)

    def remote(src, dst, send, recv, **where):
        return pltpu.make_async_remote_copy(
            src_ref=src, dst_ref=dst, send_sem=send, recv_sem=recv,
            device_id=where, device_id_type=MESH,
        )

    swap_tok = remote(tok_h, tok.at[1], tok_send.at[0], tok_recv.at[0], tp=1 - tp)
    swap_gain = remote(gain, gain_o, tok_send.at[1], tok_recv.at[1], tp=1 - tp)
    swap_tok.start()
    swap_gain.start()

    bx[...] = jnp.zeros_like(bx)
    cx[...] = jnp.zeros_like(cx)
    zr, zi = zoh_of(rate[...], angle[...])
    for g in range(groups):
        q, k = g // per, g % per
        r, l = k * ch, k * entries
        gr, gi = zr[g : g + 1, :], zi[g : g + 1, :]
        b0, b1 = b_in[0, g], b_in[1, g]
        bx[q, r : r + ch, l : l + entries] = (gr * b0 - gi * b1).astype(BF16)
        bx[q, r : r + ch, wide + l : wide + l + entries] = (gr * b1 + gi * b0).astype(BF16)
        cx[q, r : r + ch, l : l + entries] = c_out[0, g].astype(BF16)
        cx[q, r : r + ch, wide + l : wide + l + entries] = (-c_out[1, g]).astype(BF16)

    parts = jnp.concatenate(split3(jnp.exp(shift[...])), axis=0)
    count = parts.shape[0]
    pad = -count % 128
    if pad:
        parts = jnp.concatenate([parts, jnp.zeros((pad, rows), F32)], axis=0)
    parts = parts.T.astype(BF16)
    kk = lax.broadcasted_iota(jnp.int32, (count + pad, 128), 0)
    cc = lax.broadcasted_iota(jnp.int32, (count + pad, 128), 1)
    for j in range(lines):
        owner = (cc + j * 128) // entries
        spread = jnp.where((kk < count) & (lax.rem(kk, groups) == owner), 1.0, 0.0).astype(BF16)
        e_s[pl.ds(j, rows, stride=lines), :] = dot(parts, spread)

    def packed(ref):
        left = ref[pl.ds(0, lines, stride=2), :]
        right = ref[pl.ds(1, lines, stride=2), :]
        return jnp.concatenate([left, right], axis=1)

    rate_p, angle_p = packed(rate), packed(angle)
    size = jnp.exp(-rate_p)
    lam_re, lam_im = size * jnp.cos(angle_p), size * jnp.sin(angle_p)

    copies[0].wait()
    floats = tok[0].astype(F32)
    sc[0] = (floats * gain[...].astype(F32)).astype(BF16)
    squares = jnp.sum(floats * floats, axis=1, keepdims=True)
    copies[1].wait()
    total = dot(sc[0], w[0, 0])
    swap_tok.wait()
    swap_gain.wait()
    floats = tok[1].astype(F32)
    sc[1] = (floats * gain_o[...].astype(F32)).astype(BF16)
    squares = squares + jnp.sum(floats * floats, axis=1, keepdims=True)
    inv = lax.rsqrt(squares / (2 * half) + 1e-06)
    copies[2].wait()
    total = total + dot(sc[1], w[0, 1])
    u = (total * inv).astype(BF16)
    for q in range(blocks):
        drive = dot(u[:, q * 128 : (q + 1) * 128], bx[q])
        for k in range(wide // 128):
            j = q * (wide // 128) + k
            d_re[pl.ds(j, rows, stride=lines), :] = drive[:, k * 128 : (k + 1) * 128]
            d_im[pl.ds(j, rows, stride=lines), :] = drive[:, wide + k * 128 : wide + (k + 1) * 128]

    def advance(n, s_re, s_im):
        here = pl.ds(pl.multiple_of(n * lines, lines), lines)
        decay = e_s[here, :]
        a_re, a_im = lam_re * decay, lam_im * decay
        new_re = (a_re * s_re - a_im * s_im) + d_re[here, :]
        new_im = (a_re * s_im + a_im * s_re) + d_im[here, :]
        return here, decay, new_re, new_im

    unroll = 8
    nil = jnp.zeros((lines, 128), F32)

    def first_pass(t, carry):
        s_re, s_im, kept = carry
        for k in range(unroll):
            _, decay, s_re, s_im = advance(t * unroll + k, s_re, s_im)
            kept = kept * decay
        return s_re, s_im, kept

    s_re, s_im, kept = lax.fori_loop(0, rows // unroll, first_pass, (nil, nil, nil + 1.0))
    mine1[0] = s_re
    mine1[1] = s_im
    mine1[2] = kept
    slots1[0, 0] = s_re
    slots1[0, 1] = s_im
    slots1[0, 2] = kept
    sends1 = []
    for k, peer in enumerate(peers1, 1):
        sends1.append(
            remote(mine1, slots1.at[k], ph1_send.at[k], ph1_recv.at[k], sp=peer)
        )
        sends1[-1].start()

    def power(re, im, exponent):
        out_re, out_im = None, None
        while exponent:
            if exponent % 2:
                if out_re is None:
                    out_re, out_im = re, im
                else:
                    out_re, out_im = out_re * re - out_im * im, out_re * im + out_im * re
            re, im = re * re - im * im, 2.0 * re * im
            exponent //= 2
        return out_re, out_im

    lam1_re, lam1_im = power(lam_re, lam_im, rows)
    lam2_re, lam2_im = power(lam1_re, lam1_im, n1)

    def project(number):
        copies[1 + 2 * number].wait()
        value = dot(sc[0], w[number, 0])
        copies[2 + 2 * number].wait()
        value = value + dot(sc[1], w[number, 1])
        return (value * inv).astype(BF16).astype(F32)

    cg = project(1)
    gated[8:, :] = cg * project(2)
    swap_halo = remote(
        gated.at[pl.ds(rows, 8), :], halo, halo_send.at[0], halo_recv.at[0], sp=nxt
    )
    swap_halo.start()

    def follow(state, slot, p_re, p_im, use):
        re, im = state
        keep = slot[2]
        a_re, a_im = p_re * keep, p_im * keep
        new_re = a_re * re - a_im * im + slot[0]
        new_im = a_re * im + a_im * re + slot[1]
        if use is None:
            return new_re, new_im
        return jnp.where(use, new_re, re), jnp.where(use, new_im, im)

    for send in sends1:
        send.wait()
    state, kept = (nil, nil), nil + 1.0
    for member in range(n1):
        slot = slots1[lax.rem(inner - member + n1, n1)]
        state = follow(state, slot, lam1_re, lam1_im, None)
        kept = kept * slot[2]
    mine2[0], mine2[1], mine2[2] = state[0], state[1], kept
    slots2[0, 0], slots2[0, 1], slots2[0, 2] = state[0], state[1], kept
    sends2 = []
    for k, peer in enumerate(peers2, 1):
        sends2.append(
            remote(mine2, slots2.at[k], ph2_send.at[k], ph2_recv.at[k], sp=peer)
        )
        sends2[-1].start()

    bg = project(3)
    swap_halo.wait()
    gated[0:8, :] = jnp.where(sp > 0, halo[...], 0.0)
    conv = None
    for tap in range(KERNEL):
        lo = 8 - (KERNEL - 1) + tap
        term = gated[lo : lo + rows, :] * taps[tap : tap + 1, :]
        conv = term if conv is None else conv + term
    conv = bg * conv

    def head_norm(values, gains, head):
        r = lax.broadcasted_iota(jnp.int32, (128, 128), 0) // head
        c = lax.broadcasted_iota(jnp.int32, (128, 128), 1) // head
        mean = jnp.where(r == c, 1.0 / head, 0.0).astype(BF16)
        pieces = []
        for q in range(values.shape[1] // 128):
            v = values[:, q * 128 : (q + 1) * 128]
            scale = lax.rsqrt(dot((v * v).astype(BF16), mean) + 1e-06)
            pieces.append((v * scale * gains[:, q * 128 : (q + 1) * 128]).astype(BF16))
        return jnp.concatenate(pieces, axis=1)

    conv_b = head_norm(conv, cgain[...], CONVOLUTION_CHAN)
    copies[9].wait()
    acc[...] = dot(conv_b, woc[...])

    for send in sends2:
        send.wait()
    state = (packed(init.at[0]), packed(init.at[1]))
    for member in range(n2 - 1):
        slot = slots2[lax.rem(outer - member + n2, n2)]
        state = follow(state, slot, lam2_re, lam2_im, member < outer)
    for member in range(n1 - 1):
        slot = slots1[lax.rem(inner - member + n1, n1)]
        state = follow(state, slot, lam1_re, lam1_im, member < inner)

    def second_pass(t, carry):
        s_re, s_im = carry
        for k in range(unroll):
            here, _, s_re, s_im = advance(t * unroll + k, s_re, s_im)
            d_re[here, :] = s_re
            d_im[here, :] = s_im
        return s_re, s_im

    lax.fori_loop(0, rows // unroll, second_pass, state)
    for q in range(blocks):
        pieces = []
        for ref in (d_re, d_im):
            for k in range(wide // 128):
                j = q * (wide // 128) + k
                pieces.append(ref[pl.ds(j, rows, stride=lines), :].astype(BF16))
        y = dot_nt(jnp.concatenate(pieces, axis=1), cx[q])
        cols = slice(q * 128, (q + 1) * 128)
        pre = y + skip[:, cols] * u[:, cols].astype(F32)
        act = 0.5 * pre * (1.0 + lax.erf(pre * (0.5**0.5)))
        ssm_b[:, cols] = head_norm(act, sgain[:, cols], ch)

    copies[10].wait()
    total_cols = wos.shape[1]
    chunks = part_r.shape[0]
    step = total_cols // chunks
    part_rows = rows // 2
    own = pl.ds(pl.multiple_of(tp * part_rows, part_rows), part_rows)
    other = pl.ds(pl.multiple_of((1 - tp) * part_rows, part_rows), part_rows)
    sends = []
    for c in range(chunks):
        cols = slice(c * step, (c + 1) * step)
        part_s[c] = (acc[:, cols] + dot(ssm_b[...], wos[:, cols])).astype(BF16)
        sends.append(
            remote(part_s.at[c, other], part_r.at[c], out_send.at[c], out_recv.at[c], tp=1 - tp)
        )
        sends[-1].start()
    for c in range(chunks):
        sends[c].wait()
        cols = slice(c * step, (c + 1) * step)
        out[:, cols] = (part_s[c, own].astype(F32) + part_r[c].astype(F32)).astype(BF16)


def body(
    nsp,
    tokens, in_gain, w_input, w_bgate, w_cgate, w_value, decay_rate, angle, decay_shift,
    b_input, c_output, init, skip_gain, ssm_gain, conv_gain, conv_taps, w_out_ssm, w_out_conv,
):
    rows, half = tokens.shape
    groups, entries = decay_rate.shape
    lines = groups * entries // 128
    ch = c_output.shape[2]
    inner = w_input.shape[1]
    blocks = groups // (128 // ch)
    wide = (128 // ch) * entries
    n1 = inner_size(nsp)
    n2 = nsp // n1
    total_cols = w_out_ssm.shape[1]
    chunks = 4
    vmem = pl.BlockSpec(memory_space=pltpu.VMEM)
    hbm = pl.BlockSpec(memory_space=pl.ANY)
    dma = pltpu.SemaphoreType.DMA
    return pl.pallas_call(
        functools.partial(kernel, (nsp, n1, n2)),
        out_shape=jax.ShapeDtypeStruct((rows // 2, total_cols), BF16),
        in_specs=[hbm, vmem, hbm, hbm, hbm, hbm] + [vmem] * 10 + [hbm, hbm],
        out_specs=vmem,
        scratch_shapes=[
            pltpu.VMEM((2, rows, half), BF16),
            pltpu.VMEM(in_gain.shape, BF16),
            pltpu.VMEM((4, 2, half, inner), BF16),
            pltpu.VMEM(w_out_ssm.shape, BF16),
            pltpu.VMEM(w_out_conv.shape, BF16),
            pltpu.VMEM((2, rows, half), BF16),
            pltpu.VMEM((blocks, 128, 2 * wide), BF16),
            pltpu.VMEM((blocks, 128, 2 * wide), BF16),
            pltpu.VMEM((rows * lines, 128), F32),
            pltpu.VMEM((rows * lines, 128), F32),
            pltpu.VMEM((rows * lines, 128), F32),
            pltpu.VMEM((rows + 8, w_bgate.shape[1]), F32),
            pltpu.VMEM((8, w_bgate.shape[1]), F32),
            pltpu.VMEM((rows, total_cols), F32),
            pltpu.VMEM((rows, inner), BF16),
            pltpu.VMEM((3, lines, 128), F32),
            pltpu.VMEM((n1, 3, lines, 128), F32),
            pltpu.VMEM((3, lines, 128), F32),
            pltpu.VMEM((n2, 3, lines, 128), F32),
            pltpu.VMEM((chunks, rows, total_cols // chunks), BF16),
            pltpu.VMEM((chunks, rows // 2, total_cols // chunks), BF16),
            dma((11,)),
            dma((2,)),
            dma((2,)),
            dma((n1,)),
            dma((n1,)),
            dma((n2,)),
            dma((n2,)),
            dma((1,)),
            dma((1,)),
            dma((chunks,)),
            dma((chunks,)),
        ],
        compiler_params=pltpu.CompilerParams(
            collective_id=0, has_side_effects=True, vmem_limit_bytes=56 * 1024 * 1024
        ),
    )(
        tokens, in_gain, w_input, w_bgate, w_cgate, w_value, decay_rate, angle, decay_shift,
        b_input.transpose(0, 1, 3, 2), c_output, init,
        skip_gain.reshape(1, -1), ssm_gain.reshape(1, -1), conv_gain.reshape(1, -1),
        conv_taps, w_out_ssm, w_out_conv,
    )


def solution(mesh):
    return jax.shard_map(
        functools.partial(body, mesh.shape["sp"]),
        mesh=mesh,
        in_specs=(
            P("sp", "tp"),
            P(None, "tp"),
            P(None, "tp"),
            P(None, "tp"),
            P(None, "tp"),
            P(None, "tp"),
            P("tp", None),
            P("tp", None),
            P("tp", "sp"),
            P(None, "tp", None, None),
            P(None, "tp", None, None),
            P(None, "tp", None),
            P("tp"),
            P("tp"),
            P("tp"),
            P(None, "tp"),
            P("tp", None),
            P("tp", None),
        ),
        out_specs=P(("sp", "tp"), None),
        check_vma=False,
    )
```

```python
import functools

import jax
import jax.numpy as jnp
from jax import lax
from jax.experimental import pallas as pl
from jax.experimental.pallas import tpu as pltpu
from jax.sharding import PartitionSpec as P

CONVOLUTION_CHAN = 64
KERNEL = 3
MESH = pl.DeviceIdType.MESH
F32 = jnp.float32
BF16 = jnp.bfloat16


def inner_size(count):
    size = 1
    while size * size < count:
        size *= 2
    return size


def dot(a, b):
    return jnp.dot(a, b, preferred_element_type=F32)


def dot_nt(a, b):
    return lax.dot_general(a, b, (((1,), (1,)), ((), ())), preferred_element_type=F32)


def expm1_of(x):
    series = x * (1 + x / 2 * (1 + x / 3 * (1 + x / 4 * (1 + x / 5 * (1 + x / 6)))))
    return jnp.where(jnp.abs(x) < 0.125, series, jnp.exp(x) - 1)


def zoh_of(rate, angle):
    real_part = expm1_of(-rate) * jnp.cos(angle) - 2.0 * jnp.sin(0.5 * angle) ** 2
    imag_part = jnp.exp(-rate) * jnp.sin(angle)
    denom = rate * rate + angle * angle
    return (
        (imag_part * angle - real_part * rate) / denom,
        -(imag_part * rate + real_part * angle) / denom,
    )


def split3(x):
    hi = x.astype(BF16).astype(F32)
    mid = (x - hi).astype(BF16).astype(F32)
    return hi, mid, x - hi - mid


def kernel(
    sizes,
    tok_h, gain, w_in_h, w_bg_h, w_cg_h, w_va_h, rate, angle, shift, b_h, c_h, init,
    skip, sgain, cgain, taps, wos_h, woc_h,
    out_own, out_oth,
    tok, b_in, c_out, gain_o, w, wos, woc, sc, bx, cx, e_s, d_re, d_im, gated, halo, acc, ssm_b,
    mine1, slots1, mine2, slots2, part_s,
    loc_sem, tok_send, tok_recv, ph1_send, ph1_recv, ph2_send, ph2_recv, halo_send, halo_recv,
    out_send, out_recv, own_sem,
):
    nsp, n1, n2 = sizes
    sp, tp = lax.axis_index("sp"), lax.axis_index("tp")
    rows, half = tok_h.shape
    groups, entries = rate.shape
    ch = c_h.shape[2]
    per = 128 // ch
    width = groups * entries
    lines = width // 128
    blocks = groups // per
    wide = per * entries
    inner, outer = lax.rem(sp, n1), lax.div(sp, n1)
    nxt, prv = lax.rem(sp + 1, nsp), lax.rem(sp + nsp - 1, nsp)

    def half_of(ref, which):
        start = (tp if which == 0 else 1 - tp) * half
        return ref.at[pl.ds(pl.multiple_of(start, half), half), :]

    copies = [pltpu.make_async_copy(tok_h, tok.at[0], loc_sem.at[0])]
    for number, ref in enumerate((w_in_h, w_cg_h, w_va_h, w_bg_h)):
        for which in range(2):
            copies.append(
                pltpu.make_async_copy(
                    half_of(ref, which), w.at[number, which], loc_sem.at[len(copies)]
                )
            )
    copies.append(pltpu.make_async_copy(woc_h, woc, loc_sem.at[len(copies)]))
    copies.append(pltpu.make_async_copy(wos_h, wos, loc_sem.at[len(copies)]))
    copies.append(pltpu.make_async_copy(b_h, b_in, loc_sem.at[len(copies)]))
    copies.append(pltpu.make_async_copy(c_h, c_out, loc_sem.at[len(copies)]))
    for k in (0, 1, 11, 2, 12, 3, 4):
        copies[k].start()

    peers1 = [outer * n1 + lax.rem(inner + k, n1) for k in range(1, n1)]
    peers2 = [lax.rem(outer + k, n2) * n1 + inner for k in range(1, n2)]
    barrier = pltpu.get_barrier_semaphore()
    pl.semaphore_signal(barrier, inc=1, device_id={"tp": 1 - tp}, device_id_type=MESH)
    for peer in peers1 + peers2 + [nxt, prv]:
        pl.semaphore_signal(barrier, inc=1, device_id={"sp": peer}, device_id_type=MESH)

    def remote(src, dst, send, recv, **where):
        return pltpu.make_async_remote_copy(
            src_ref=src, dst_ref=dst, send_sem=send, recv_sem=recv,
            device_id=where, device_id_type=MESH,
        )

    swap_tok = remote(tok.at[0], tok.at[1], tok_send.at[0], tok_recv.at[0], tp=1 - tp)
    swap_gain = remote(gain, gain_o, tok_send.at[1], tok_recv.at[1], tp=1 - tp)
    copies[0].wait()
    floats = tok[0].astype(F32)
    sc[0] = (floats * gain[...].astype(F32)).astype(BF16)
    squares = jnp.sum(floats * floats, axis=1, keepdims=True)
    parts = jnp.concatenate(split3(jnp.exp(shift[...])), axis=0)
    count = parts.shape[0]
    pad = -count % 128
    if pad:
        parts = jnp.concatenate([parts, jnp.zeros((pad, rows), F32)], axis=0)
    parts = parts.T.astype(BF16)
    kk = lax.broadcasted_iota(jnp.int32, (count + pad, 128), 0)
    cc = lax.broadcasted_iota(jnp.int32, (count + pad, 128), 1)
    for j in range(lines):
        owner = (cc + j * 128) // entries
        spread = jnp.where((kk < count) & (lax.rem(kk, groups) == owner), 1.0, 0.0).astype(BF16)
        e_s[pl.ds(j, rows, stride=lines), :] = dot(parts, spread)

    def packed(ref):
        left = ref[pl.ds(0, lines, stride=2), :]
        right = ref[pl.ds(1, lines, stride=2), :]
        return jnp.concatenate([left, right], axis=1)

    rate_p, angle_p = packed(rate), packed(angle)
    size = jnp.exp(-rate_p)
    lam_re, lam_im = size * jnp.cos(angle_p), size * jnp.sin(angle_p)

    pl.semaphore_wait(barrier, 1 + len(peers1) + len(peers2) + 2)
    swap_tok.start()
    swap_gain.start()

    bx[...] = jnp.zeros_like(bx)
    cx[...] = jnp.zeros_like(cx)
    copies[11].wait()
    copies[12].wait()
    zr, zi = zoh_of(rate[...], angle[...])
    for g in range(groups):
        q, k = g // per, g % per
        r, l = k * ch, k * entries
        gr, gi = zr[g : g + 1, :], zi[g : g + 1, :]
        b0, b1 = b_in[0, g], b_in[1, g]
        bx[q, r : r + ch, l : l + entries] = (gr * b0 - gi * b1).astype(BF16)
        bx[q, r : r + ch, wide + l : wide + l + entries] = (gr * b1 + gi * b0).astype(BF16)
        cx[q, r : r + ch, l : l + entries] = c_out[0, g].astype(BF16)
        cx[q, r : r + ch, wide + l : wide + l + entries] = (-c_out[1, g]).astype(BF16)

    copies[1].wait()
    total = dot(sc[0], w[0, 0])
    for k in range(5, 11):
        copies[k].start()
    swap_tok.wait()
    swap_gain.wait()
    floats = tok[1].astype(F32)
    sc[1] = (floats * gain_o[...].astype(F32)).astype(BF16)
    squares = squares + jnp.sum(floats * floats, axis=1, keepdims=True)
    inv = lax.rsqrt(squares / (2 * half) + 1e-06)
    copies[2].wait()
    total = total + dot(sc[1], w[0, 1])
    u = (total * inv).astype(BF16)
    for q in range(blocks):
        drive = dot(u[:, q * 128 : (q + 1) * 128], bx[q])
        for k in range(wide // 128):
            j = q * (wide // 128) + k
            d_re[pl.ds(j, rows, stride=lines), :] = drive[:, k * 128 : (k + 1) * 128]
            d_im[pl.ds(j, rows, stride=lines), :] = drive[:, wide + k * 128 : wide + (k + 1) * 128]

    def advance(n, s_re, s_im):
        here = pl.ds(pl.multiple_of(n * lines, lines), lines)
        decay = e_s[here, :]
        a_re, a_im = lam_re * decay, lam_im * decay
        new_re = (a_re * s_re - a_im * s_im) + d_re[here, :]
        new_im = (a_re * s_im + a_im * s_re) + d_im[here, :]
        return here, decay, new_re, new_im

    unroll = 32
    nil = jnp.zeros((lines, 128), F32)

    def first_pass(t, carry):
        s_re, s_im, kept = carry
        for k in range(unroll):
            _, decay, s_re, s_im = advance(t * unroll + k, s_re, s_im)
            kept = kept * decay
        return s_re, s_im, kept

    s_re, s_im, kept = lax.fori_loop(0, rows // unroll, first_pass, (nil, nil, nil + 1.0))
    mine1[0] = s_re
    mine1[1] = s_im
    mine1[2] = kept
    slots1[0, 0] = s_re
    slots1[0, 1] = s_im
    slots1[0, 2] = kept
    sends1 = []
    for k, peer in enumerate(peers1, 1):
        sends1.append(
            remote(mine1, slots1.at[k], ph1_send.at[k], ph1_recv.at[k], sp=peer)
        )
        sends1[-1].start()

    def power(re, im, exponent):
        out_re, out_im = None, None
        while exponent:
            if exponent % 2:
                if out_re is None:
                    out_re, out_im = re, im
                else:
                    out_re, out_im = out_re * re - out_im * im, out_re * im + out_im * re
            re, im = re * re - im * im, 2.0 * re * im
            exponent //= 2
        return out_re, out_im

    lam1_re, lam1_im = power(lam_re, lam_im, rows)
    lam2_re, lam2_im = power(lam1_re, lam1_im, n1)

    def project(number):
        copies[1 + 2 * number].wait()
        value = dot(sc[0], w[number, 0])
        copies[2 + 2 * number].wait()
        value = value + dot(sc[1], w[number, 1])
        return (value * inv).astype(BF16).astype(F32)

    cg = project(1)
    gated[8:, :] = cg * project(2)
    swap_halo = remote(
        gated.at[pl.ds(rows, 8), :], halo, halo_send.at[0], halo_recv.at[0], sp=nxt
    )
    swap_halo.start()

    def follow(state, slot, p_re, p_im, use):
        re, im = state
        keep = slot[2]
        a_re, a_im = p_re * keep, p_im * keep
        new_re = a_re * re - a_im * im + slot[0]
        new_im = a_re * im + a_im * re + slot[1]
        if use is None:
            return new_re, new_im
        return jnp.where(use, new_re, re), jnp.where(use, new_im, im)

    for send in sends1:
        send.wait()
    state, kept = (nil, nil), nil + 1.0
    for member in range(n1):
        slot = slots1[lax.rem(inner - member + n1, n1)]
        state = follow(state, slot, lam1_re, lam1_im, None)
        kept = kept * slot[2]
    mine2[0], mine2[1], mine2[2] = state[0], state[1], kept
    slots2[0, 0], slots2[0, 1], slots2[0, 2] = state[0], state[1], kept
    sends2 = []
    for k, peer in enumerate(peers2, 1):
        sends2.append(
            remote(mine2, slots2.at[k], ph2_send.at[k], ph2_recv.at[k], sp=peer)
        )
        sends2[-1].start()

    bg = project(3)
    swap_halo.wait()
    gated[0:8, :] = jnp.where(sp > 0, halo[...], 0.0)
    conv = None
    for tap in range(KERNEL):
        lo = 8 - (KERNEL - 1) + tap
        term = gated[lo : lo + rows, :] * taps[tap : tap + 1, :]
        conv = term if conv is None else conv + term
    conv = bg * conv

    def head_norm(values, gains, head):
        r = lax.broadcasted_iota(jnp.int32, (128, 128), 0) // head
        c = lax.broadcasted_iota(jnp.int32, (128, 128), 1) // head
        mean = jnp.where(r == c, 1.0 / head, 0.0).astype(BF16)
        pieces = []
        for q in range(values.shape[1] // 128):
            v = values[:, q * 128 : (q + 1) * 128]
            scale = lax.rsqrt(dot((v * v).astype(BF16), mean) + 1e-06)
            pieces.append((v * scale * gains[:, q * 128 : (q + 1) * 128]).astype(BF16))
        return jnp.concatenate(pieces, axis=1)

    conv_b = head_norm(conv, cgain[...], CONVOLUTION_CHAN)
    copies[9].wait()
    acc[...] = dot(conv_b, woc[...])

    for send in sends2:
        send.wait()
    state = (packed(init.at[0]), packed(init.at[1]))
    for member in range(n2 - 1):
        slot = slots2[lax.rem(outer - member + n2, n2)]
        state = follow(state, slot, lam2_re, lam2_im, member < outer)
    for member in range(n1 - 1):
        slot = slots1[lax.rem(inner - member + n1, n1)]
        state = follow(state, slot, lam1_re, lam1_im, member < inner)

    def second_pass(t, carry):
        s_re, s_im = carry
        for k in range(unroll):
            here, _, s_re, s_im = advance(t * unroll + k, s_re, s_im)
            d_re[here, :] = s_re
            d_im[here, :] = s_im
        return s_re, s_im

    lax.fori_loop(0, rows // unroll, second_pass, state)
    for q in range(blocks):
        pieces = []
        for ref in (d_re, d_im):
            for k in range(wide // 128):
                j = q * (wide // 128) + k
                pieces.append(ref[pl.ds(j, rows, stride=lines), :].astype(BF16))
        y = dot_nt(jnp.concatenate(pieces, axis=1), cx[q])
        cols = slice(q * 128, (q + 1) * 128)
        pre = y + skip[:, cols] * u[:, cols].astype(F32)
        act = 0.5 * pre * (1.0 + lax.erf(pre * (0.5**0.5)))
        ssm_b[:, cols] = head_norm(act, sgain[:, cols], ch)

    copies[10].wait()
    total_cols = wos.shape[1]
    chunks = part_s.shape[0]
    step = total_cols // chunks
    part_rows = rows // 2
    own = pl.ds(pl.multiple_of(tp * part_rows, part_rows), part_rows)
    other = pl.ds(pl.multiple_of((1 - tp) * part_rows, part_rows), part_rows)
    sends, keeps = [], []
    for c in range(chunks):
        cols = slice(c * step, (c + 1) * step)
        part_s[c] = (acc[:, cols] + dot(ssm_b[...], wos[:, cols])).astype(BF16)
        sends.append(
            remote(
                part_s.at[c, other], out_oth.at[:, pl.ds(c * step, step)],
                out_send.at[c], out_recv.at[c], tp=1 - tp,
            )
        )
        sends[-1].start()
        keeps.append(
            pltpu.make_async_copy(
                part_s.at[c, own], out_own.at[:, pl.ds(c * step, step)], own_sem.at[c]
            )
        )
        keeps[-1].start()
    for c in range(chunks):
        keeps[c].wait()
        sends[c].wait()


def body(
    nsp,
    tokens, in_gain, w_input, w_bgate, w_cgate, w_value, decay_rate, angle, decay_shift,
    b_input, c_output, init, skip_gain, ssm_gain, conv_gain, conv_taps, w_out_ssm, w_out_conv,
):
    rows, half = tokens.shape
    groups, entries = decay_rate.shape
    lines = groups * entries // 128
    ch = c_output.shape[2]
    inner = w_input.shape[1]
    blocks = groups // (128 // ch)
    wide = (128 // ch) * entries
    n1 = inner_size(nsp)
    n2 = nsp // n1
    total_cols = w_out_ssm.shape[1]
    chunks = 4
    vmem = pl.BlockSpec(memory_space=pltpu.VMEM)
    hbm = pl.BlockSpec(memory_space=pl.ANY)
    dma = pltpu.SemaphoreType.DMA
    result = jax.ShapeDtypeStruct((rows // 2, total_cols), BF16)
    own, other = pl.pallas_call(
        functools.partial(kernel, (nsp, n1, n2)),
        out_shape=(result, result),
        in_specs=[hbm, vmem, hbm, hbm, hbm, hbm] + [vmem] * 3 + [hbm, hbm] + [vmem] * 5 + [hbm, hbm],
        out_specs=(hbm, hbm),
        scratch_shapes=[
            pltpu.VMEM((2, rows, half), BF16),
            pltpu.VMEM((2, groups, ch, entries), F32),
            pltpu.VMEM(c_output.shape, F32),
            pltpu.VMEM(in_gain.shape, BF16),
            pltpu.VMEM((4, 2, half, inner), BF16),
            pltpu.VMEM(w_out_ssm.shape, BF16),
            pltpu.VMEM(w_out_conv.shape, BF16),
            pltpu.VMEM((2, rows, half), BF16),
            pltpu.VMEM((blocks, 128, 2 * wide), BF16),
            pltpu.VMEM((blocks, 128, 2 * wide), BF16),
            pltpu.VMEM((rows * lines, 128), F32),
            pltpu.VMEM((rows * lines, 128), F32),
            pltpu.VMEM((rows * lines, 128), F32),
            pltpu.VMEM((rows + 8, w_bgate.shape[1]), F32),
            pltpu.VMEM((8, w_bgate.shape[1]), F32),
            pltpu.VMEM((rows, total_cols), F32),
            pltpu.VMEM((rows, inner), BF16),
            pltpu.VMEM((3, lines, 128), F32),
            pltpu.VMEM((n1, 3, lines, 128), F32),
            pltpu.VMEM((3, lines, 128), F32),
            pltpu.VMEM((n2, 3, lines, 128), F32),
            pltpu.VMEM((chunks, rows, total_cols // chunks), BF16),
            dma((13,)),
            dma((2,)),
            dma((2,)),
            dma((n1,)),
            dma((n1,)),
            dma((n2,)),
            dma((n2,)),
            dma((1,)),
            dma((1,)),
            dma((chunks,)),
            dma((chunks,)),
            dma((chunks,)),
        ],
        compiler_params=pltpu.CompilerParams(
            collective_id=0, has_side_effects=True, vmem_limit_bytes=56 * 1024 * 1024
        ),
    )(
        tokens, in_gain, w_input, w_bgate, w_cgate, w_value, decay_rate, angle, decay_shift,
        b_input.transpose(0, 1, 3, 2), c_output, init,
        skip_gain.reshape(1, -1), ssm_gain.reshape(1, -1), conv_gain.reshape(1, -1),
        conv_taps, w_out_ssm, w_out_conv,
    )
    return (own.astype(F32) + other.astype(F32)).astype(BF16)


def solution(mesh):
    return jax.shard_map(
        functools.partial(body, mesh.shape["sp"]),
        mesh=mesh,
        in_specs=(
            P("sp", "tp"),
            P(None, "tp"),
            P(None, "tp"),
            P(None, "tp"),
            P(None, "tp"),
            P(None, "tp"),
            P("tp", None),
            P("tp", None),
            P("tp", "sp"),
            P(None, "tp", None, None),
            P(None, "tp", None, None),
            P(None, "tp", None),
            P("tp"),
            P("tp"),
            P("tp"),
            P(None, "tp"),
            P("tp", None),
            P("tp", None),
        ),
        out_specs=P(("sp", "tp"), None),
        check_vma=False,
    )
```
